32 devices in a mesh: sp: 8 (over z, x), tp: 4 (over y, core).
Axes of the slice: x: 2, y: 2, z: 4, core: 2. Of those that a mesh axis runs over, the one named last changes fastest.
Arguments:
- mixer_input: bfloat16 [4096, 2048], P('sp', 'tp'), may hold values from -6 to 6
- residual: bfloat16 [4096, 2048], P(('sp', 'tp')), may hold values from -6 to 6
- log_step: float32 [128], P('tp'), may hold values from -3.9 to -2.3
- rate_real: float32 [128, 64], P('tp'), may hold values from -1.5 to 0, as said below
- rate_imag: float32 [128, 64], P('tp'), may hold values from 2 to 30
- damping: float32 [4096, 128], P('sp', 'tp'), may hold values from -2 to 0, as said below
- in_map: float32 [2, 128, 64, 16], P(None, 'tp'), may hold values from -1 to 1
- out_map: float32 [2, 128, 16, 64], P(None, 'tp'), may hold values from -0.75 to 0.75
- skip: float32 [2048], P('tp'), may hold values from -3 to 3
- w_out: bfloat16 [2048, 2048], P('tp'), may hold values from -0.125 to 0.125
- norm_gain: float32 [2048], replicated, may hold values from 0.1 to 1.9
- w_act: bfloat16 [2048, 5632], P('sp', 'tp'), may hold values from -0.125 to 0.125
- w_lin: bfloat16 [2048, 5632], P('sp', 'tp'), may hold values from -0.125 to 0.125
- conv_taps: float32 [2, 3, 5632], P(None, None, 'tp'), may hold values from -3.5 to 3.5
- w_down: bfloat16 [5632, 2048], P('tp', 'sp'), may hold values from -0.078125 to 0.078125
Outputs:
- layer_out: bfloat16 [4096, 2048], P(('sp', 'tp'))
The draws below stay inside these ranges and needn't reach their ends.
Inputs may be any that keep to these rules, and one draw needn't show every extreme that they name: `rate_real`: all entries negative. `damping`: all entries at most zero.
All inputs are finite; a program needn't handle non-finite values.
Results may differ from the reference program's by a relative error of at most 0.02.
Values may be sent and summed in bfloat16 or wider, within the bound.
A program may use at most 192 MiB of HBM per device.

```python
import math
import jax
import jax.numpy as jnp
from jax import lax

D = 2048
GROUP = 16
SSM_CLUSTERS = 128
STATE = 64
FF = 5632
CONV = 3
TOK_DEV = 512
SERIES_SPAN = 4096
N_TP = 4


def draw_rate_real(key, part):
    pick_key, fast_key, slow_key = jax.random.split(jax.random.fold_in(key, 11), 3)
    slow_share = 0.5
    slow_groups = jax.random.bernoulli(pick_key, slow_share, (SSM_CLUSTERS,))
    fast_rates = -jnp.exp(jax.random.uniform(fast_key, (SSM_CLUSTERS, STATE), jnp.float32, math.log(0.25), math.log(1.5)))
    slow_rates = -jnp.exp(jax.random.uniform(slow_key, (SSM_CLUSTERS, STATE), jnp.float32, 0.0, math.log(4.0))) / SERIES_SPAN
    return jnp.where(slow_groups[:, None], slow_rates, fast_rates)


def draw_damping(key, part):
    rate_key, spike_index_seed, amplitude_seed = jax.random.split(jax.random.fold_in(key, 23), 3)
    block_rates = jnp.exp(jax.random.uniform(rate_key, (SERIES_SPAN // TOK_DEV, SSM_CLUSTERS), jnp.float32, 0.0, math.log(4.0)))
    baseline_value = -0.2 * jnp.repeat(block_rates, TOK_DEV, axis=0) / SERIES_SPAN
    spike_indices = jax.random.randint(spike_index_seed, (2, SSM_CLUSTERS), 0, SERIES_SPAN)
    spike_falloffs = jnp.log(jax.random.uniform(amplitude_seed, (2, SSM_CLUSTERS), jnp.float32, 0.55, 0.8))
    element_indices = jnp.arange(SERIES_SPAN)[:, None]
    spike_occurrences = jnp.where(element_indices == spike_indices[0][None, :], spike_falloffs[0][None, :], 0.0)
    spike_occurrences = spike_occurrences + jnp.where(element_indices == spike_indices[1][None, :], spike_falloffs[1][None, :], 0.0)
    return (baseline_value + spike_occurrences).astype(jnp.float32)


def levels(stream_key, dims, pieces, smallest, high):
    loudness = 1.0
    for axis_at, parts in pieces:
        heights = jax.random.uniform(jax.random.fold_in(jax.random.fold_in(stream_key, 6), axis_at), (parts,), jnp.float32, smallest / len(pieces), high / len(pieces))
        loudness = loudness * jnp.repeat(jnp.exp(heights), dims[axis_at] // parts).reshape((-1,) + (1,) * (len(dims) - 1 - axis_at))
    return loudness


def scatter_about(rng, extent, spread, most, cuts=(), dtype=jnp.bfloat16):
    gain = levels(rng, extent, cuts, -0.22, 0.18) if cuts else 1.0
    values = jax.random.normal(rng, extent, jnp.float32) * spread * gain
    return jnp.minimum(jnp.maximum(values, -most), most).astype(dtype)


def setup_inputs(seed: int = 0) -> dict:
    keys = jax.random.split(jax.random.key(seed), 16)
    return {
        "mixer_input": scatter_about(keys[0], (SERIES_SPAN, D), 1.0, 6.0, ((0, 8), (1, 4))),
        "residual": scatter_about(keys[1], (SERIES_SPAN, D), 1.0, 6.0, ((0, 32),)),
        "log_step": jnp.clip(-3.9 + 1.6000001 * jax.random.uniform(keys[2], (SSM_CLUSTERS,), jnp.float32) ** levels(keys[2], (SSM_CLUSTERS,), ((0, 4),), -0.2, 0.2), -3.9, -2.3),
        "rate_real": draw_rate_real(jax.random.fold_in(keys[15], 71), 0),
        "rate_imag": jnp.clip(jnp.exp(math.log(30.0) - 2.7080502 * jax.random.uniform(keys[4], (SSM_CLUSTERS, STATE), jnp.float32) ** levels(keys[4], (SSM_CLUSTERS, STATE), ((0, 4),), -0.2, 0.2)), 2.0, 30.0),
        "damping": draw_damping(jax.random.fold_in(keys[15], 71), 0),
        "in_map": scatter_about(keys[6], (2, SSM_CLUSTERS, STATE, GROUP), (2 * GROUP) ** -0.5, 1.0, ((1, 4),), jnp.float32),
        "out_map": scatter_about(keys[7], (2, SSM_CLUSTERS, GROUP, STATE), STATE ** -0.5, 0.75, ((1, 4),), jnp.float32),
        "skip": scatter_about(keys[8], (D,), 0.5, 3.0, ((0, 4),), jnp.float32),
        "w_out": scatter_about(keys[9], (D, D), D ** -0.5, 0.125, ((0, 4),)),
        "norm_gain": jnp.clip(1.0 + 0.18 * jax.random.normal(keys[10], (D,), jnp.float32), 0.1, 1.9),
        "w_act": scatter_about(keys[11], (D, FF), D ** -0.5, 0.125, ((0, 8), (1, 4))),
        "w_lin": scatter_about(keys[12], (D, FF), D ** -0.5, 0.125, ((0, 8), (1, 4))),
        "conv_taps": scatter_about(keys[13], (2, CONV, FF), CONV ** -0.5, 3.5, ((2, 4),), jnp.float32),
        "w_down": scatter_about(keys[14], (FF, D), FF ** -0.5, 0.078125, ((0, 4), (1, 8))),
    }


def combine(earlier, later):
    a1r, a1i, b1r, b1i = earlier
    a2r, a2i, b2r, b2i = later
    return (a2r * a1r - a2i * a1i, a2r * a1i + a2i * a1r, a2r * b1r - a2i * b1i + b2r, a2r * b1i + a2i * b1r + b2i)

def one_group(packed):
    group_in, group_damp, bbar_re, bbar_im, log_rate, angle_step, cmap_re, cmap_im, skip_group = packed
    hi = lax.Precision.HIGHEST
    drive_re = jnp.dot(group_in, bbar_re.T, precision=hi)
    drive_im = jnp.dot(group_in, bbar_im.T, precision=hi)
    magnitude = jnp.exp(log_rate[None, :] + group_damp[:, None])
    trans_re = magnitude * jnp.cos(angle_step)[None, :]
    trans_im = magnitude * jnp.sin(angle_step)[None, :]
    scanned = lax.associative_scan(combine, (trans_re, trans_im, drive_re, drive_im), axis=0)
    state_re, state_im = (scanned[2], scanned[3])
    return jnp.dot(state_re, cmap_re.T, precision=hi) - jnp.dot(state_im, cmap_im.T, precision=hi) + skip_group[None, :] * group_in

def rounded_sum(total, partial_value):
    return total + lax.optimization_barrier(partial_value.astype(jnp.bfloat16)).astype(jnp.float32)

def reference(mixer_input, residual, log_step, rate_real, rate_imag, damping, in_map, out_map, skip, w_out, norm_gain, w_act, w_lin, conv_taps, w_down):
    seq_len = mixer_input.shape[0]
    step_size = jnp.exp(log_step)[:, None]
    log_rate = rate_real * step_size
    angle_step = rate_imag * step_size
    magnitude = jnp.exp(log_rate)
    abar_re = magnitude * jnp.cos(angle_step)
    abar_im = magnitude * jnp.sin(angle_step)
    denominator = rate_real * rate_real + rate_imag * rate_imag
    minus_one = abar_re - 1.0
    factor_re = (minus_one * rate_real + abar_im * rate_imag) / denominator
    factor_im = (abar_im * rate_real - minus_one * rate_imag) / denominator
    bbar_re = factor_re[..., None] * in_map[0] - factor_im[..., None] * in_map[1]
    bbar_im = factor_re[..., None] * in_map[1] + factor_im[..., None] * in_map[0]
    inputs = jnp.transpose(mixer_input.astype(jnp.float32).reshape(seq_len, SSM_CLUSTERS, GROUP), (1, 0, 2))
    outputs = lax.map(one_group, (inputs, damping.T, bbar_re, bbar_im, log_rate, angle_step, out_map[0], out_map[1], skip.reshape(SSM_CLUSTERS, GROUP)))
    mixed = jnp.transpose(outputs, (1, 0, 2)).reshape(seq_len, D)
    activated = jax.nn.gelu(mixed).astype(jnp.bfloat16)
    width_tp = D // N_TP
    projected = jnp.zeros((seq_len, D), jnp.float32)
    for shard in range(N_TP):
        window = slice(shard * width_tp, (shard + 1) * width_tp)
        partial_value = jnp.dot(activated[:, window], w_out[window], preferred_element_type=jnp.float32)
        projected = rounded_sum(projected, partial_value)
    stream = (residual.astype(jnp.float32) + projected).astype(jnp.bfloat16)
    stream_f = stream.astype(jnp.float32)
    normed = (stream_f * lax.rsqrt(lax.optimization_barrier(jnp.mean(stream_f * stream_f, axis=-1, keepdims=True)) + 1e-06) * norm_gain).astype(jnp.bfloat16)
    hidden_tp = FF // N_TP
    channel_sum = jnp.zeros((seq_len, D), jnp.float32)
    for shard in range(N_TP):
        window = slice(shard * hidden_tp, (shard + 1) * hidden_tp)
        act_pre = jnp.dot(normed, w_act[:, window], preferred_element_type=jnp.float32).astype(jnp.bfloat16)
        lin_pre = jnp.dot(normed, w_lin[:, window], preferred_element_type=jnp.float32).astype(jnp.bfloat16)
        padding = jnp.zeros((CONV - 1, hidden_tp), jnp.float32)
        act_pad = jnp.concatenate([padding, act_pre.astype(jnp.float32)], axis=0)
        lin_pad = jnp.concatenate([padding, lin_pre.astype(jnp.float32)], axis=0)
        act_conv = jnp.zeros((seq_len, hidden_tp), jnp.float32)
        lin_conv = jnp.zeros((seq_len, hidden_tp), jnp.float32)
        for offset in range(CONV):
            act_conv = act_conv + conv_taps[0, offset, window][None, :] * act_pad[offset:offset + seq_len]
            lin_conv = lin_conv + conv_taps[1, offset, window][None, :] * lin_pad[offset:offset + seq_len]
        hidden = (jax.nn.silu(act_conv) * lin_conv).astype(jnp.bfloat16)
        partial_value = jnp.dot(hidden, w_down[window], preferred_element_type=jnp.float32)
        channel_sum = rounded_sum(channel_sum, partial_value)
    return (stream.astype(jnp.float32) + channel_sum).astype(jnp.bfloat16)
```

```python
import functools

import jax
import jax.numpy as jnp
from jax import lax
from jax.experimental import pallas as pl
from jax.experimental.pallas import tpu as pltpu
from jax.sharding import PartitionSpec as P

CONV = 3
SUB = 8
LANE_BLOCK = 512
MESH = pl.DeviceIdType.MESH


def complex_power(re, im, exponent):
    out = None
    while exponent:
        if exponent & 1:
            out = (
                (re, im)
                if out is None
                else (out[0] * re - out[1] * im, out[0] * im + out[1] * re)
            )
        exponent >>= 1
        if exponent:
            re, im = (re * re - im * im, 2.0 * re * im)
    return out


def mixer_kernel(
    ring,
    states,
    x_ref,
    damp_ref,
    abar_re_ref,
    abar_im_ref,
    in_re_ref,
    in_im_ref,
    out_re_ref,
    out_im_ref,
    skip_ref,
    w_out_ref,
    proj_ref,
    growth,
    state_re,
    state_im,
    begin_re,
    begin_im,
    outbox,
    inbox,
    send_sem,
    recv_sem,
):
    bf16, f32 = (jnp.bfloat16, jnp.float32)
    me = lax.axis_index("sp")
    barrier = pltpu.get_barrier_semaphore()
    for apart in range(1, ring):
        peer = lax.rem(me + apart, ring)
        pl.semaphore_signal(barrier, inc=1, device_id={"sp": peer}, device_id_type=MESH)
    tokens = x_ref.shape[0]
    lanes = growth.shape[1]
    steps = tokens // SUB
    rows = lax.broadcasted_iota(jnp.int32, (tokens, tokens), 0)
    cols = lax.broadcasted_iota(jnp.int32, (tokens, tokens), 1)
    spread = (cols == (rows % SUB) * steps + rows // SUB).astype(bf16)
    gather = (rows == (cols % SUB) * steps + cols // SUB).astype(bf16)
    x_perm = jnp.dot(spread, x_ref[...], preferred_element_type=f32).astype(bf16)
    factor = jnp.exp(damp_ref[...])
    high = factor.astype(bf16)
    rest = factor - high.astype(f32)
    middle = rest.astype(bf16)
    low = (rest - middle.astype(f32)).astype(bf16)
    groups = factor.shape[1]
    pick = (
        lax.broadcasted_iota(jnp.int32, (groups, lanes), 1) // states
        == lax.broadcasted_iota(jnp.int32, (groups, lanes), 0)
    ).astype(bf16)
    total = None
    for part in (high, middle, low):
        moved = jnp.dot(spread, part, preferred_element_type=f32).astype(bf16)
        wide = jnp.dot(moved, pick, preferred_element_type=f32)
        total = wide if total is None else total + wide
    growth[...] = total
    blocks = in_re_ref.shape[0]
    width = in_re_ref.shape[1]
    span = in_re_ref.shape[2]
    for b in range(blocks):
        piece = x_perm[:, b * width : (b + 1) * width]
        state_re[:, b * span : (b + 1) * span] = jnp.dot(
            piece, in_re_ref[b], preferred_element_type=f32
        )
        state_im[:, b * span : (b + 1) * span] = jnp.dot(
            piece, in_im_ref[b], preferred_element_type=f32
        )

    def advance(start, keep, cut, re, im, a_re, a_im):
        row = pl.multiple_of(start * SUB, SUB)
        grow = growth[pl.ds(row, SUB), cut]
        re, im = (re * grow, im * grow)
        new_re = a_re * re - a_im * im + state_re[pl.ds(row, SUB), cut]
        new_im = a_re * im + a_im * re + state_im[pl.ds(row, SUB), cut]
        if keep:
            state_re[pl.ds(row, SUB), cut] = new_re
            state_im[pl.ds(row, SUB), cut] = new_im
        return (new_re, new_im, grow)

    total_re, total_im = complex_power(abar_re_ref[...], abar_im_ref[...], steps)
    local = []
    for lane in range(0, lanes, LANE_BLOCK):
        cut = slice(lane, lane + LANE_BLOCK)
        a_re = jnp.broadcast_to(abar_re_ref[:, cut], (SUB, LANE_BLOCK))
        a_im = jnp.broadcast_to(abar_im_ref[:, cut], (SUB, LANE_BLOCK))

        def body(step, carry):
            re, im, grown = carry
            re, im, grow = advance(step, False, cut, re, im, a_re, a_im)
            return (re, im, grown * grow)

        zero = jnp.zeros((SUB, LANE_BLOCK), f32)
        re, im, grown = lax.fori_loop(
            0, steps, body, (zero, zero, jnp.ones((SUB, LANE_BLOCK), f32)), unroll=4
        )
        local.append((re, im, grown * total_re[:, cut], grown * total_im[:, cut]))
    fin_re, fin_im, jump_re, jump_im = [
        jnp.concatenate([item[k] for item in local], axis=1) for k in range(4)
    ]
    at_re, at_im = (fin_re[0:1], fin_im[0:1])
    all_re, all_im = (jump_re[0:1], jump_im[0:1])
    for c in range(1, SUB):
        j_re, j_im = (jump_re[c : c + 1], jump_im[c : c + 1])
        at_re, at_im = (
            j_re * at_re - j_im * at_im + fin_re[c : c + 1],
            j_re * at_im + j_im * at_re + fin_im[c : c + 1],
        )
        all_re, all_im = (j_re * all_re - j_im * all_im, j_re * all_im + j_im * all_re)
    outbox[0:1, :] = at_re
    outbox[1:2, :] = at_im
    outbox[2:3, :] = all_re
    outbox[3:4, :] = all_im
    pl.semaphore_wait(barrier, ring - 1)
    copies = []
    for apart in range(1, ring):
        copy = pltpu.make_async_remote_copy(
            src_ref=outbox,
            dst_ref=inbox.at[apart],
            send_sem=send_sem.at[apart],
            recv_sem=recv_sem.at[apart],
            device_id={"sp": lax.rem(me + apart, ring)},
            device_id_type=MESH,
        )
        copy.start()
        copies.append(copy)
    for copy in copies:
        copy.wait()
    at_re = jnp.zeros((1, lanes), f32)
    at_im = jnp.zeros((1, lanes), f32)
    for apart in range(ring - 1, 0, -1):
        f_re, f_im = (inbox[apart, 0:1, :], inbox[apart, 1:2, :])
        j_re, j_im = (inbox[apart, 2:3, :], inbox[apart, 3:4, :])
        valid = me >= apart
        new_re = j_re * at_re - j_im * at_im + f_re
        new_im = j_re * at_im + j_im * at_re + f_im
        at_re = jnp.where(valid, new_re, at_re)
        at_im = jnp.where(valid, new_im, at_im)
    for c in range(SUB):
        begin_re[c : c + 1, :] = at_re
        begin_im[c : c + 1, :] = at_im
        if c < SUB - 1:
            j_re, j_im = (jump_re[c : c + 1], jump_im[c : c + 1])
            at_re, at_im = (
                j_re * at_re - j_im * at_im + fin_re[c : c + 1],
                j_re * at_im + j_im * at_re + fin_im[c : c + 1],
            )
    for lane in range(0, lanes, LANE_BLOCK):
        cut = slice(lane, lane + LANE_BLOCK)
        a_re = jnp.broadcast_to(abar_re_ref[:, cut], (SUB, LANE_BLOCK))
        a_im = jnp.broadcast_to(abar_im_ref[:, cut], (SUB, LANE_BLOCK))

        def body(step, carry):
            re, im, _ = advance(step, True, cut, *carry, a_re, a_im)
            return (re, im)

        lax.fori_loop(0, steps, body, (begin_re[:, cut], begin_im[:, cut]), unroll=4)
    pieces = []
    for b in range(blocks):
        cut = slice(b * span, (b + 1) * span)
        here = slice(b * width, (b + 1) * width)
        mixed = (
            jnp.dot(state_re[:, cut].astype(bf16), out_re_ref[b], preferred_element_type=f32)
            - jnp.dot(state_im[:, cut].astype(bf16), out_im_ref[b], preferred_element_type=f32)
            + skip_ref[:, here] * x_perm[:, here].astype(f32)
        )
        pieces.append(jax.nn.gelu(mixed).astype(bf16))
    activated = jnp.dot(
        gather, jnp.concatenate(pieces, axis=1), preferred_element_type=f32
    ).astype(bf16)
    columns = w_out_ref.shape[1]
    piece = min(512, columns)

    def project(k, _):
        there = pl.ds(pl.multiple_of(k * piece, piece), piece)
        proj_ref[:, there] = jnp.dot(
            activated, w_out_ref[:, there], preferred_element_type=f32
        ).astype(bf16)
        return 0

    lax.fori_loop(0, columns // piece, project, 0)


def block_diagonal(parts, per_block):
    groups, rows, cols = parts.shape
    blocks = groups // per_block
    eye = jnp.eye(per_block, dtype=parts.dtype)
    wide = (
        parts.reshape(blocks, per_block, rows, 1, cols) * eye[None, :, None, :, None]
    )
    return wide.reshape(blocks, per_block * rows, per_block * cols).astype(jnp.bfloat16)


def state_projection(
    mixer_input, log_step, rate_real, rate_imag, damping, in_map, out_map, skip, w_out
):
    tokens_here, channels = mixer_input.shape
    groups_here, states = rate_real.shape
    group_width = channels // groups_here
    step_size = jnp.exp(log_step)[:, None]
    log_rate = rate_real * step_size
    angle_step = rate_imag * step_size
    magnitude = jnp.exp(log_rate)
    abar_re = magnitude * jnp.cos(angle_step)
    abar_im = magnitude * jnp.sin(angle_step)
    denominator = rate_real * rate_real + rate_imag * rate_imag
    minus_one = abar_re - 1.0
    factor_re = (minus_one * rate_real + abar_im * rate_imag) / denominator
    factor_im = (abar_im * rate_real - minus_one * rate_imag) / denominator
    bbar_re = factor_re[..., None] * in_map[0] - factor_im[..., None] * in_map[1]
    bbar_im = factor_re[..., None] * in_map[1] + factor_im[..., None] * in_map[0]
    per_block = 128 // group_width
    lanes = groups_here * states
    ring = lax.axis_size("sp")
    vmem = pl.BlockSpec(memory_space=pltpu.VMEM)
    f32 = jnp.float32
    return pl.pallas_call(
        functools.partial(mixer_kernel, ring, states),
        out_shape=jax.ShapeDtypeStruct((tokens_here, w_out.shape[1]), jnp.bfloat16),
        in_specs=[vmem] * 10,
        out_specs=vmem,
        scratch_shapes=[
            pltpu.VMEM((tokens_here, lanes), f32),
            pltpu.VMEM((tokens_here, lanes), f32),
            pltpu.VMEM((tokens_here, lanes), f32),
            pltpu.VMEM((SUB, lanes), f32),
            pltpu.VMEM((SUB, lanes), f32),
            pltpu.VMEM((4, lanes), f32),
            pltpu.VMEM((ring, 4, lanes), f32),
            pltpu.SemaphoreType.DMA((ring,)),
            pltpu.SemaphoreType.DMA((ring,)),
        ],
        compiler_params=pltpu.CompilerParams(
            collective_id=0, has_side_effects=True, vmem_limit_bytes=56 * 1024 * 1024
        ),
        cost_estimate=pl.CostEstimate(
            flops=20_000_000_000, bytes_accessed=8_000_000, transcendentals=0
        ),
        name="state_projection",
    )(
        mixer_input,
        damping,
        abar_re.reshape(1, lanes),
        abar_im.reshape(1, lanes),
        block_diagonal(jnp.swapaxes(bbar_re, 1, 2), per_block),
        block_diagonal(jnp.swapaxes(bbar_im, 1, 2), per_block),
        block_diagonal(jnp.swapaxes(out_map[0], 1, 2), per_block),
        block_diagonal(jnp.swapaxes(out_map[1], 1, 2), per_block),
        skip.reshape(1, channels),
        w_out,
    )


def from_partner(block, axis, apart):
    count = lax.axis_size(axis)
    route = []
    for low in range(count):
        high = low | 1 << apart
        if high != low and high < count:
            route += [(low, high), (high, low)]
    return lax.ppermute(block, axis, route)


def from_behind(value, axis, steps):
    count = lax.axis_size(axis)
    initial, last = (max(0, -steps), min(count, count - steps))
    return lax.ppermute(value, axis, [(source, source + steps) for source in range(initial, last)])


def normalize(stream, norm_gain):
    stream_f = stream.astype(jnp.float32)
    scale = lax.rsqrt(jnp.mean(stream_f * stream_f, axis=-1, keepdims=True) + 1e-06)
    return (stream_f * scale * norm_gain).astype(jnp.bfloat16)


def causal_conv(act_pre, lin_pre, previous, taps):
    row_count, width = act_pre.shape
    act_pad = jnp.concatenate([previous[0], act_pre], axis=0).astype(jnp.float32)
    lin_pad = jnp.concatenate([previous[1], lin_pre], axis=0).astype(jnp.float32)
    act_conv = jnp.zeros((row_count, width), jnp.float32)
    lin_conv = jnp.zeros((row_count, width), jnp.float32)
    for offset in range(CONV):
        act_conv = act_conv + taps[0, offset][None, :] * act_pad[offset : offset + row_count]
        lin_conv = lin_conv + taps[1, offset][None, :] * lin_pad[offset : offset + row_count]
    return (jax.nn.silu(act_conv) * lin_conv).astype(jnp.bfloat16)


def per_device(
    mixer_input,
    residual,
    log_step,
    rate_real,
    rate_imag,
    damping,
    in_map,
    out_map,
    skip,
    w_out,
    norm_gain,
    w_act,
    w_lin,
    conv_taps,
    w_down,
):
    tokens_here = mixer_input.shape[0]
    hidden_here = w_act.shape[1]
    partial_projection = state_projection(
        mixer_input, log_step, rate_real, rate_imag, damping, in_map, out_map, skip, w_out
    )
    projected = lax.psum_scatter(
        partial_projection,
        "tp",
        scatter_dimension=0,
        tiled=True,
    ).astype(jnp.float32)
    stream = (residual.astype(jnp.float32) + projected).astype(jnp.bfloat16)
    normed_all = lax.all_gather(normalize(stream, norm_gain), "tp", axis=0, tiled=True)
    parity = lax.axis_index("sp") % 2
    half = hidden_here // 2
    copies = lax.axis_size("sp") // 2

    def outgoing_rows(weight):
        paired = jnp.concatenate([weight[:, :half], weight[:, half:]], axis=0)
        return jnp.tile(paired, (copies, 1))

    act_half, lin_half = (
        lax.all_to_all(outgoing_rows(w_act), "sp", split_axis=0, concat_axis=0, tiled=True),
        lax.all_to_all(outgoing_rows(w_lin), "sp", split_axis=0, concat_axis=0, tiled=True),
    )
    paired_down = jnp.concatenate([w_down[:half], w_down[half:]], axis=1)
    down_half = lax.all_to_all(
        jnp.tile(paired_down, (1, copies)), "sp", split_axis=1, concat_axis=1, tiled=True
    )
    partner = from_partner(normed_all, "sp", 0)
    first = jnp.where(parity == 0, normed_all, partner)
    second = jnp.where(parity == 0, partner, normed_all)
    normed_pair = jnp.concatenate([first, second], axis=0)
    act_pre = jnp.dot(normed_pair, act_half, preferred_element_type=jnp.float32).astype(
        jnp.bfloat16
    )
    lin_pre = jnp.dot(normed_pair, lin_half, preferred_element_type=jnp.float32).astype(
        jnp.bfloat16
    )
    edge = 2 * tokens_here - (CONV - 1)
    previous = from_behind((act_pre[edge:], lin_pre[edge:]), "sp", 2)
    taps = lax.dynamic_slice_in_dim(conv_taps, parity * half, half, 2)
    hidden = causal_conv(act_pre, lin_pre, previous, taps)
    partial_value = jnp.dot(hidden, down_half, preferred_element_type=jnp.float32)
    mine = lax.dynamic_slice_in_dim(partial_value, parity * tokens_here, tokens_here, 0)
    other = lax.dynamic_slice_in_dim(partial_value, (1 - parity) * tokens_here, tokens_here, 0)
    block_total = mine + from_partner(other, "sp", 0)
    channel_sum = lax.psum_scatter(
        block_total.astype(jnp.bfloat16), "tp", scatter_dimension=0, tiled=True
    ).astype(jnp.float32)
    return (stream.astype(jnp.float32) + channel_sum).astype(jnp.bfloat16)


def solution(mesh):
    in_specs = (
        P("sp", "tp"),
        P(("sp", "tp"), None),
        P("tp"),
        P("tp", None),
        P("tp", None),
        P("sp", "tp"),
        P(None, "tp", None, None),
        P(None, "tp", None, None),
        P("tp"),
        P("tp", None),
        P(),
        P("sp", "tp"),
        P("sp", "tp"),
        P(None, None, "tp"),
        P("tp", "sp"),
    )
    out_specs = P(("sp", "tp"), None)
    return jax.shard_map(
        per_device, mesh=mesh, in_specs=in_specs, out_specs=out_specs, check_vma=False
    )
```

```python
import functools

import jax
import jax.numpy as jnp
from jax import lax
from jax.experimental import pallas as pl
from jax.experimental.pallas import tpu as pltpu
from jax.sharding import PartitionSpec as P

CONV = 3
SUB = 8
LANE_BLOCK = 512
MESH = pl.DeviceIdType.MESH


def complex_power(re, im, exponent):
    out = None
    while exponent:
        if exponent & 1:
            out = (
                (re, im)
                if out is None
                else (out[0] * re - out[1] * im, out[0] * im + out[1] * re)
            )
        exponent >>= 1
        if exponent:
            re, im = (re * re - im * im, 2.0 * re * im)
    return out


def greet(barrier, ring, team):
    me, mine = (lax.axis_index("sp"), lax.axis_index("tp"))
    partner = me + 1 - 2 * (me % 2)
    peers = [(lax.rem(me + apart, ring), mine) for apart in range(1, ring)]
    for apart in range(1, team):
        other = lax.rem(mine + apart, team)
        peers += [(me, other), (partner, other)]
    for at_sp, at_tp in peers:
        pl.semaphore_signal(
            barrier, inc=1, device_id={"sp": at_sp, "tp": at_tp}, device_id_type=MESH
        )
    return len(peers)


def remote(src, dst, send, recv, at_sp, at_tp):
    return pltpu.make_async_remote_copy(
        src_ref=src,
        dst_ref=dst,
        send_sem=send,
        recv_sem=recv,
        device_id={"sp": at_sp, "tp": at_tp},
        device_id_type=MESH,
    )


def diagonal(compact, copies, height, states):
    tall = jnp.concatenate([compact] * copies, axis=0)
    rows = lax.broadcasted_iota(jnp.int32, tall.shape, 0) // height
    cols = lax.broadcasted_iota(jnp.int32, tall.shape, 1) // states
    return jnp.where(rows == cols, tall, 0.0).astype(jnp.bfloat16)


def entry_kernel(
    ring,
    team,
    states,
    x_ref,
    damp_ref,
    abar_re_ref,
    abar_im_ref,
    factor_re_ref,
    factor_im_ref,
    in_ref,
    out_ref,
    skip_ref,
    w_out_ref,
    residual_ref,
    gain_ref,
    w_act_ref,
    w_lin_ref,
    w_down_ref,
    stream_ref,
    pair_ref,
    act_ref,
    lin_ref,
    down_ref,
    growth,
    state_re,
    state_im,
    begin_re,
    begin_im,
    outbox,
    inbox,
    proj,
    rs_in,
    stage,
    stage_down,
    send_sem,
    recv_sem,
    rs_send,
    rs_recv,
    ag_send,
    ag_recv,
    hop_send,
    hop_recv,
    local_sem,
):
    bf16, f32 = (jnp.bfloat16, jnp.float32)
    me, mine = (lax.axis_index("sp"), lax.axis_index("tp"))
    barrier = pltpu.get_barrier_semaphore()
    greeted = greet(barrier, ring, team)
    parity = me % 2
    partner = me + 1 - 2 * parity
    circle = ring // 2
    spot = me // 2
    wide = stage.shape[2]
    shift = w_act_ref.shape[1] - wide

    def originals(side):
        cut = pl.ds(pl.multiple_of(side * shift, 128), wide)
        return [w_act_ref.at[:, cut], w_lin_ref.at[:, cut], w_down_ref.at[cut, :]]

    gathered = [act_ref, lin_ref, down_ref]
    keep = [stage.at[0], stage.at[1], stage_down]
    loads = [
        pltpu.make_async_copy(src, dst, local_sem.at[k])
        for k, (src, dst) in enumerate(zip(originals(parity), keep))
    ]
    for load in loads:
        load.start()
    pl.semaphore_wait(barrier, greeted)
    far, near = (circle // 2, (circle - 1) // 2)
    hops = {"x": 0}
    for name, count in (("or", far), ("ol", near), ("pl", far), ("pr", near)):
        for hop in range(1, count + 1):
            hops[name, hop] = len(hops)
    hop_copies = {}

    def send_blocks(key, sources, slot, target):
        made = []
        for k in range(3):
            index = hops[key] * 3 + k
            copy = remote(
                sources[k],
                gathered[k].at[slot],
                hop_send.at[index],
                hop_recv.at[index],
                target,
                mine,
            )
            copy.start()
            made.append(copy)
        hop_copies[key] = made

    def hop_on(name, hop):
        step = 1 if name[1] == "r" else circle - 1
        target = ((spot + step) % circle) * 2 + parity
        origin = ((spot + (hop - 1) * (circle - step)) % circle) * 2
        if name[0] == "o":
            slot = origin + parity
            sources = originals(parity) if hop == 1 else [ref.at[slot] for ref in gathered]
        else:
            slot = origin + 1 - parity
            sources = [ref.at[slot] for ref in gathered]
        send_blocks((name, hop), sources, slot, target)

    def landed(key):
        for copy in hop_copies[key]:
            copy.wait_recv()

    send_blocks("x", originals(1 - parity), me, partner)
    hop_on("or", 1)
    if near:
        hop_on("ol", 1)
    tokens = x_ref.shape[0]
    lanes = growth.shape[1]
    steps = tokens // SUB
    rows = lax.broadcasted_iota(jnp.int32, (tokens, tokens), 0)
    cols = lax.broadcasted_iota(jnp.int32, (tokens, tokens), 1)
    spread = (cols == (rows % SUB) * steps + rows // SUB).astype(bf16)
    gather = (rows == (cols % SUB) * steps + cols // SUB).astype(bf16)
    x_perm = jnp.dot(spread, x_ref[...], preferred_element_type=f32).astype(bf16)
    factor = jnp.exp(damp_ref[...])
    high = factor.astype(bf16)
    rest = factor - high.astype(f32)
    middle = rest.astype(bf16)
    low = (rest - middle.astype(f32)).astype(bf16)
    groups = factor.shape[1]
    pick = (
        lax.broadcasted_iota(jnp.int32, (groups, lanes), 1) // states
        == lax.broadcasted_iota(jnp.int32, (groups, lanes), 0)
    ).astype(bf16)
    total = None
    for part in (high, middle, low):
        moved = jnp.dot(spread, part, preferred_element_type=f32).astype(bf16)
        spanned = jnp.dot(moved, pick, preferred_element_type=f32)
        total = spanned if total is None else total + spanned
    growth[...] = total
    height = in_ref.shape[1]
    width = 128
    per_block = width // height
    span = per_block * states
    blocks = groups // per_block
    for b in range(blocks):
        piece = x_perm[:, b * width : (b + 1) * width]
        cut = slice(b * span, (b + 1) * span)
        f_re, f_im = (factor_re_ref[:, cut], factor_im_ref[:, cut])
        m_re, m_im = (in_ref[0, :, cut], in_ref[1, :, cut])
        bbar_re = diagonal(f_re * m_re - f_im * m_im, per_block, height, states)
        bbar_im = diagonal(f_re * m_im + f_im * m_re, per_block, height, states)
        state_re[:, cut] = jnp.dot(piece, bbar_re, preferred_element_type=f32)
        state_im[:, cut] = jnp.dot(piece, bbar_im, preferred_element_type=f32)

    def advance(start, keep, cut, re, im, a_re, a_im):
        row = pl.multiple_of(start * SUB, SUB)
        grow = growth[pl.ds(row, SUB), cut]
        re, im = (re * grow, im * grow)
        new_re = a_re * re - a_im * im + state_re[pl.ds(row, SUB), cut]
        new_im = a_re * im + a_im * re + state_im[pl.ds(row, SUB), cut]
        if keep:
            state_re[pl.ds(row, SUB), cut] = new_re
            state_im[pl.ds(row, SUB), cut] = new_im
        return (new_re, new_im, grow)

    total_re, total_im = complex_power(abar_re_ref[...], abar_im_ref[...], steps)
    local = []
    for lane in range(0, lanes, LANE_BLOCK):
        cut = slice(lane, lane + LANE_BLOCK)
        a_re = jnp.broadcast_to(abar_re_ref[:, cut], (SUB, LANE_BLOCK))
        a_im = jnp.broadcast_to(abar_im_ref[:, cut], (SUB, LANE_BLOCK))

        def body(step, carry):
            re, im, grown = carry
            re, im, grow = advance(step, False, cut, re, im, a_re, a_im)
            return (re, im, grown * grow)

        zero = jnp.zeros((SUB, LANE_BLOCK), f32)
        re, im, grown = lax.fori_loop(
            0, steps, body, (zero, zero, jnp.ones((SUB, LANE_BLOCK), f32)), unroll=4
        )
        local.append((re, im, grown * total_re[:, cut], grown * total_im[:, cut]))
    fin_re, fin_im, jump_re, jump_im = [
        jnp.concatenate([item[k] for item in local], axis=1) for k in range(4)
    ]
    at_re, at_im = (fin_re[0:1], fin_im[0:1])
    all_re, all_im = (jump_re[0:1], jump_im[0:1])
    for c in range(1, SUB):
        j_re, j_im = (jump_re[c : c + 1], jump_im[c : c + 1])
        at_re, at_im = (
            j_re * at_re - j_im * at_im + fin_re[c : c + 1],
            j_re * at_im + j_im * at_re + fin_im[c : c + 1],
        )
        all_re, all_im = (j_re * all_re - j_im * all_im, j_re * all_im + j_im * all_re)
    outbox[0:1, :] = at_re
    outbox[1:2, :] = at_im
    outbox[2:3, :] = all_re
    outbox[3:4, :] = all_im
    copies = []
    for apart in range(1, ring):
        copy = remote(
            outbox,
            inbox.at[apart],
            send_sem.at[apart],
            recv_sem.at[apart],
            lax.rem(me + apart, ring),
            mine,
        )
        copy.start()
        copies.append(copy)
    for copy in copies:
        copy.wait()
    at_re = jnp.zeros((1, lanes), f32)
    at_im = jnp.zeros((1, lanes), f32)
    for apart in range(ring - 1, 0, -1):
        f_re, f_im = (inbox[apart, 0:1, :], inbox[apart, 1:2, :])
        j_re, j_im = (inbox[apart, 2:3, :], inbox[apart, 3:4, :])
        valid = me >= apart
        new_re = j_re * at_re - j_im * at_im + f_re
        new_im = j_re * at_im + j_im * at_re + f_im
        at_re = jnp.where(valid, new_re, at_re)
        at_im = jnp.where(valid, new_im, at_im)
    for c in range(SUB):
        begin_re[c : c + 1, :] = at_re
        begin_im[c : c + 1, :] = at_im
        if c < SUB - 1:
            j_re, j_im = (jump_re[c : c + 1], jump_im[c : c + 1])
            at_re, at_im = (
                j_re * at_re - j_im * at_im + fin_re[c : c + 1],
                j_re * at_im + j_im * at_re + fin_im[c : c + 1],
            )
    for lane in range(0, lanes, LANE_BLOCK):
        cut = slice(lane, lane + LANE_BLOCK)
        a_re = jnp.broadcast_to(abar_re_ref[:, cut], (SUB, LANE_BLOCK))
        a_im = jnp.broadcast_to(abar_im_ref[:, cut], (SUB, LANE_BLOCK))

        def body(step, carry):
            re, im, _ = advance(step, True, cut, *carry, a_re, a_im)
            return (re, im)

        lax.fori_loop(0, steps, body, (begin_re[:, cut], begin_im[:, cut]), unroll=4)

    def across(state, compact):
        return lax.dot_general(
            state,
            diagonal(compact, per_block, height, states),
            (((1,), (1,)), ((), ())),
            preferred_element_type=f32,
        )

    pieces = []
    for b in range(blocks):
        cut = slice(b * span, (b + 1) * span)
        here = slice(b * width, (b + 1) * width)
        mixed = (
            across(state_re[:, cut].astype(bf16), out_ref[0, :, cut])
            - across(state_im[:, cut].astype(bf16), out_ref[1, :, cut])
            + skip_ref[:, here] * x_perm[:, here].astype(f32)
        )
        pieces.append(jax.nn.gelu(mixed).astype(bf16))
    activated = jnp.dot(
        gather, jnp.concatenate(pieces, axis=1), preferred_element_type=f32
    ).astype(bf16)
    columns = w_out_ref.shape[1]
    piece = min(512, columns)

    def project(k, _):
        there = pl.ds(pl.multiple_of(k * piece, piece), piece)
        proj[:, there] = jnp.dot(
            activated, w_out_ref[:, there], preferred_element_type=f32
        ).astype(bf16)
        return 0

    lax.fori_loop(0, columns // piece, project, 0)
    share = tokens // team
    sums = []
    for apart in range(1, team):
        other = lax.rem(mine + apart, team)
        copy = remote(
            proj.at[pl.ds(pl.multiple_of(other * share, share), share), :],
            rs_in.at[apart],
            rs_send.at[apart],
            rs_recv.at[apart],
            me,
            other,
        )
        copy.start()
        sums.append(copy)
    stores = []
    for k in range(3):
        loads[k].wait()
        store = pltpu.make_async_copy(keep[k], gathered[k].at[me], local_sem.at[3 + k])
        store.start()
        stores.append(store)
    landed("x")
    if near:
        hop_on("pr", 1)
    hop_on("pl", 1)
    if far > 1:
        landed(("or", 1))
        hop_on("or", 2)
    for copy in sums:
        copy.wait()
    total = proj[pl.ds(pl.multiple_of(mine * share, share), share), :].astype(f32)
    for apart in range(1, team):
        total = total + rs_in[apart].astype(f32)
    stream = (residual_ref[...].astype(f32) + total).astype(bf16)
    stream_ref[...] = stream
    stream = stream.astype(f32)
    scale = lax.rsqrt(jnp.mean(stream * stream, axis=-1, keepdims=True) + 1e-06)
    place = pl.ds(pl.multiple_of(parity * tokens + mine * share, share), share)
    pair_ref[place, :] = (stream * scale * gain_ref[...]).astype(bf16)
    spread_copies = []
    for k in range(2 * team - 1):
        at_sp = partner if k < team else me
        other = lax.rem(mine + (k if k < team else k - team + 1), team)
        copy = remote(
            pair_ref.at[place, :], pair_ref.at[place, :], ag_send.at[k], ag_recv.at[k], at_sp, other
        )
        copy.start()
        spread_copies.append(copy)
    if far > 1:
        landed(("pl", 1))
        hop_on("pl", 2)
    if near > 1:
        landed(("ol", 1))
        hop_on("ol", 2)
        landed(("pr", 1))
        hop_on("pr", 2)
    for hop in range(3, far + 1):
        for name in ("or", "pl", "ol", "pr"):
            if (name, hop) in hops:
                landed((name, hop - 1))
                hop_on(name, hop)
    forwarded = {("or", h) for h in range(1, far)} | {("pl", h) for h in range(1, far)}
    forwarded |= {("ol", h) for h in range(1, near)} | {("pr", h) for h in range(1, near)} | {"x"}
    for copy in spread_copies:
        copy.wait()
    for key, made in hop_copies.items():
        for copy in made:
            copy.wait_send()
            if key not in forwarded:
                copy.wait_recv()
    for store in stores:
        store.wait()


def exit_kernel(
    ring, team, hidden_ref, down_ref, stream_ref, out_ref, outbox, inbox, send_sem, recv_sem
):
    f32 = jnp.float32
    me, mine = (lax.axis_index("sp"), lax.axis_index("tp"))
    partner = me + 1 - 2 * (me % 2)
    barrier = pltpu.get_barrier_semaphore()
    rows = out_ref.shape[0]
    peers = [(partner, lax.rem(mine + apart, team)) for apart in range(team)]
    peers += [(me, lax.rem(mine + apart, team)) for apart in range(1, team)]
    for at_sp, at_tp in peers:
        pl.semaphore_signal(
            barrier, inc=1, device_id={"sp": at_sp, "tp": at_tp}, device_id_type=MESH
        )
    columns = down_ref.shape[1]
    piece = min(512, columns)

    def product(slot, at_sp, at_tp):
        start = pl.multiple_of(((at_sp % 2) * team + at_tp) * rows, rows)
        block = hidden_ref[pl.ds(start, rows), :]

        def some(k, _):
            there = pl.ds(pl.multiple_of(k * piece, piece), piece)
            outbox[slot, :, there] = jnp.dot(
                block, down_ref[:, there], preferred_element_type=f32
            ).astype(jnp.bfloat16)
            return 0

        lax.fori_loop(0, columns // piece, some, 0)

    copies = []
    order = sorted(range(len(peers)), key=lambda k: (k >= team, -(k % team)))
    for k in order:
        product(k, *peers[k])
        if not copies:
            pl.semaphore_wait(barrier, len(peers))
        copy = remote(outbox.at[k], inbox.at[k], send_sem.at[k], recv_sem.at[k], *peers[k])
        copy.start()
        copies.append(copy)
    product(len(peers), me, mine)
    for copy in copies:
        copy.wait()
    total = outbox[len(peers)].astype(f32)
    for k in range(len(peers)):
        total = total + inbox[k].astype(f32)
    out_ref[...] = (stream_ref[...].astype(f32) + total).astype(jnp.bfloat16)


def enter_layer(
    mixer_input,
    residual,
    log_step,
    rate_real,
    rate_imag,
    damping,
    in_map,
    out_map,
    skip,
    w_out,
    norm_gain,
    w_act,
    w_lin,
    w_down,
    wide,
):
    tokens_here, channels = mixer_input.shape
    groups_here, states = rate_real.shape
    step_size = jnp.exp(log_step)[:, None]
    log_rate = rate_real * step_size
    angle_step = rate_imag * step_size
    magnitude = jnp.exp(log_rate)
    abar_re = magnitude * jnp.cos(angle_step)
    abar_im = magnitude * jnp.sin(angle_step)
    denominator = rate_real * rate_real + rate_imag * rate_imag
    minus_one = abar_re - 1.0
    factor_re = (minus_one * rate_real + abar_im * rate_imag) / denominator
    factor_im = (abar_im * rate_real - minus_one * rate_imag) / denominator
    lanes = groups_here * states
    ring, team = (lax.axis_size("sp"), lax.axis_size("tp"))
    width = w_out.shape[1]
    vmem = pl.BlockSpec(memory_space=pltpu.VMEM)
    anywhere = pl.BlockSpec(memory_space=pl.ANY)
    f32, bf16 = (jnp.float32, jnp.bfloat16)
    group_width = channels // groups_here
    dma = pltpu.SemaphoreType.DMA
    hop_count = 3 * (1 + 2 * (ring // 2 - 1))
    return pl.pallas_call(
        functools.partial(entry_kernel, ring, team, states),
        out_shape=(
            jax.ShapeDtypeStruct((tokens_here // team, width), bf16),
            jax.ShapeDtypeStruct((2 * tokens_here, width), bf16),
            jax.ShapeDtypeStruct((ring, w_act.shape[0], wide), bf16),
            jax.ShapeDtypeStruct((ring, w_lin.shape[0], wide), bf16),
            jax.ShapeDtypeStruct((ring, wide, w_down.shape[1]), bf16),
        ),
        in_specs=[vmem] * 12 + [anywhere] * 3,
        out_specs=(vmem, vmem, anywhere, anywhere, anywhere),
        scratch_shapes=[
            pltpu.VMEM((tokens_here, lanes), f32),
            pltpu.VMEM((tokens_here, lanes), f32),
            pltpu.VMEM((tokens_here, lanes), f32),
            pltpu.VMEM((SUB, lanes), f32),
            pltpu.VMEM((SUB, lanes), f32),
            pltpu.VMEM((4, lanes), f32),
            pltpu.VMEM((ring, 4, lanes), f32),
            pltpu.VMEM((tokens_here, width), bf16),
            pltpu.VMEM((team, tokens_here // team, width), bf16),
            pltpu.VMEM((2, w_act.shape[0], wide), bf16),
            pltpu.VMEM((wide, w_down.shape[1]), bf16),
            dma((ring,)),
            dma((ring,)),
            dma((team,)),
            dma((team,)),
            dma((2 * team - 1,)),
            dma((2 * team - 1,)),
            dma((hop_count,)),
            dma((hop_count,)),
            dma((6,)),
        ],
        compiler_params=pltpu.CompilerParams(
            collective_id=0, has_side_effects=True, vmem_limit_bytes=56 * 1024 * 1024
        ),
        cost_estimate=pl.CostEstimate(
            flops=20_000_000_000, bytes_accessed=8_000_000, transcendentals=0
        ),
        name="enter_layer",
    )(
        mixer_input,
        damping,
        abar_re.reshape(1, lanes),
        abar_im.reshape(1, lanes),
        factor_re.reshape(1, lanes),
        factor_im.reshape(1, lanes),
        jnp.transpose(in_map, (0, 3, 1, 2)).reshape(2, group_width, lanes),
        jnp.transpose(out_map, (0, 2, 1, 3)).reshape(2, group_width, lanes),
        skip.reshape(1, channels),
        w_out,
        residual,
        norm_gain.reshape(1, width),
        w_act,
        w_lin,
        w_down,
    )


def leave_layer(hidden, down, stream):
    ring, team = (lax.axis_size("sp"), lax.axis_size("tp"))
    rows, width = stream.shape
    vmem = pl.BlockSpec(memory_space=pltpu.VMEM)
    return pl.pallas_call(
        functools.partial(exit_kernel, ring, team),
        out_shape=jax.ShapeDtypeStruct((rows, width), jnp.bfloat16),
        in_specs=[vmem] * 3,
        out_specs=vmem,
        scratch_shapes=[
            pltpu.VMEM((2 * team, rows, width), jnp.bfloat16),
            pltpu.VMEM((2 * team - 1, rows, width), jnp.bfloat16),
            pltpu.SemaphoreType.DMA((2 * team - 1,)),
            pltpu.SemaphoreType.DMA((2 * team - 1,)),
        ],
        compiler_params=pltpu.CompilerParams(
            collective_id=1, has_side_effects=True, vmem_limit_bytes=48 * 1024 * 1024
        ),
        cost_estimate=pl.CostEstimate(
            flops=20_000_000_000, bytes_accessed=8_000_000, transcendentals=0
        ),
        name="leave_layer",
    )(hidden, down, stream)


def from_behind(value, axis, steps):
    count = lax.axis_size(axis)
    initial, last = (max(0, -steps), min(count, count - steps))
    return lax.ppermute(value, axis, [(source, source + steps) for source in range(initial, last)])


def causal_conv(act_pre, lin_pre, previous, taps):
    row_count, width = act_pre.shape
    act_pad = jnp.concatenate([previous[0], act_pre], axis=0).astype(jnp.float32)
    lin_pad = jnp.concatenate([previous[1], lin_pre], axis=0).astype(jnp.float32)
    act_conv = jnp.zeros((row_count, width), jnp.float32)
    lin_conv = jnp.zeros((row_count, width), jnp.float32)
    for offset in range(CONV):
        act_conv = act_conv + taps[0, offset][None, :] * act_pad[offset : offset + row_count]
        lin_conv = lin_conv + taps[1, offset][None, :] * lin_pad[offset : offset + row_count]
    return (jax.nn.silu(act_conv) * lin_conv).astype(jnp.bfloat16)


def per_device(
    mixer_input,
    residual,
    log_step,
    rate_real,
    rate_imag,
    damping,
    in_map,
    out_map,
    skip,
    w_out,
    norm_gain,
    w_act,
    w_lin,
    conv_taps,
    w_down,
):
    tokens_here = mixer_input.shape[0]
    hidden_here = w_act.shape[1]
    wide = -(-hidden_here // 256) * 128
    parity = lax.axis_index("sp") % 2
    stream, normed_pair, act_all, lin_all, down_all = enter_layer(
        mixer_input,
        residual,
        log_step,
        rate_real,
        rate_imag,
        damping,
        in_map,
        out_map,
        skip,
        w_out,
        norm_gain,
        w_act,
        w_lin,
        w_down,
        wide,
    )
    act_half = act_all.reshape(-1, wide)
    lin_half = lin_all.reshape(-1, wide)
    down_half = jnp.transpose(down_all, (1, 0, 2)).reshape(wide, -1)
    act_pre = jnp.dot(normed_pair, act_half, preferred_element_type=jnp.float32).astype(
        jnp.bfloat16
    )
    lin_pre = jnp.dot(normed_pair, lin_half, preferred_element_type=jnp.float32).astype(
        jnp.bfloat16
    )
    edge = 2 * tokens_here - (CONV - 1)
    previous = from_behind((act_pre[edge:], lin_pre[edge:]), "sp", 2)
    taps = lax.dynamic_slice_in_dim(conv_taps, parity * (hidden_here - wide), wide, 2)
    hidden = causal_conv(act_pre, lin_pre, previous, taps)
    doubled = parity * (2 * wide - hidden_here)
    hidden = jnp.where(jnp.arange(wide)[None, :] >= doubled, hidden, jnp.zeros_like(hidden))
    return leave_layer(hidden, down_half, stream)


def solution(mesh):
    in_specs = (
        P("sp", "tp"),
        P(("sp", "tp"), None),
        P("tp"),
        P("tp", None),
        P("tp", None),
        P("sp", "tp"),
        P(None, "tp", None, None),
        P(None, "tp", None, None),
        P("tp"),
        P("tp", None),
        P(),
        P("sp", "tp"),
        P("sp", "tp"),
        P(None, None, "tp"),
        P("tp", "sp"),
    )
    out_specs = P(("sp", "tp"), None)
    return jax.shard_map(
        per_device, mesh=mesh, in_specs=in_specs, out_specs=out_specs, check_vma=False
    )
```

```python
import functools

import jax
import jax.numpy as jnp
from jax import lax
from jax.experimental import pallas as pl
from jax.experimental.pallas import tpu as pltpu
from jax.sharding import PartitionSpec as P

CONV = 3
SUB = 8
LANE_BLOCK = 512
MESH = pl.DeviceIdType.MESH


def complex_power(re, im, exponent):
    out = None
    while exponent:
        if exponent & 1:
            out = (
                (re, im)
                if out is None
                else (out[0] * re - out[1] * im, out[0] * im + out[1] * re)
            )
        exponent >>= 1
        if exponent:
            re, im = (re * re - im * im, 2.0 * re * im)
    return out


def greet(barrier, ring, team):
    me, mine = (lax.axis_index("sp"), lax.axis_index("tp"))
    partner = me + 1 - 2 * (me % 2)
    peers = [(lax.rem(me + apart, ring), mine) for apart in range(1, ring)]
    for apart in range(1, team):
        other = lax.rem(mine + apart, team)
        peers += [(me, other), (partner, other)]
    for at_sp, at_tp in peers:
        pl.semaphore_signal(
            barrier, inc=1, device_id={"sp": at_sp, "tp": at_tp}, device_id_type=MESH
        )
    return len(peers)


def remote(src, dst, send, recv, at_sp, at_tp):
    return pltpu.make_async_remote_copy(
        src_ref=src,
        dst_ref=dst,
        send_sem=send,
        recv_sem=recv,
        device_id={"sp": at_sp, "tp": at_tp},
        device_id_type=MESH,
    )


def diagonal(compact, copies, height, states):
    tall = jnp.concatenate([compact] * copies, axis=0)
    rows = lax.broadcasted_iota(jnp.int32, tall.shape, 0) // height
    cols = lax.broadcasted_iota(jnp.int32, tall.shape, 1) // states
    return jnp.where(rows == cols, tall, 0.0).astype(jnp.bfloat16)


def entry_kernel(
    ring,
    team,
    states,
    x_ref,
    damp_ref,
    abar_re_ref,
    abar_im_ref,
    factor_re_ref,
    factor_im_ref,
    in_ref,
    out_ref,
    skip_ref,
    w_out_ref,
    residual_ref,
    gain_ref,
    w_act_ref,
    w_lin_ref,
    w_down_ref,
    stream_ref,
    pair_ref,
    act_ref,
    lin_ref,
    down_ref,
    growth,
    state_re,
    state_im,
    begin_re,
    begin_im,
    outbox,
    inbox,
    proj,
    rs_in,
    stage,
    stage_down,
    send_sem,
    recv_sem,
    rs_send,
    rs_recv,
    ag_send,
    ag_recv,
    hop_send,
    hop_recv,
    local_sem,
):
    bf16, f32 = (jnp.bfloat16, jnp.float32)
    me, mine = (lax.axis_index("sp"), lax.axis_index("tp"))
    barrier = pltpu.get_barrier_semaphore()
    greeted = greet(barrier, ring, team)
    parity = me % 2
    partner = me + 1 - 2 * parity
    circle = ring // 2
    spot = me // 2
    wide = stage.shape[2]
    shift = w_act_ref.shape[1] - wide

    def originals(side):
        cut = pl.ds(pl.multiple_of(side * shift, 128), wide)
        return [w_act_ref.at[:, cut], w_lin_ref.at[:, cut], w_down_ref.at[cut, :]]

    gathered = [act_ref, lin_ref, down_ref]
    keep = [stage.at[0], stage.at[1], stage_down]
    loads = [
        pltpu.make_async_copy(src, dst, local_sem.at[k])
        for k, (src, dst) in enumerate(zip(originals(parity), keep))
    ]
    for load in loads:
        load.start()
    pl.semaphore_wait(barrier, greeted)
    far, near = (circle // 2, (circle - 1) // 2)
    hops = {"x": 0}
    for name, count in (("or", far), ("ol", near), ("pl", far), ("pr", near)):
        for hop in range(1, count + 1):
            hops[name, hop] = len(hops)
    hop_copies = {}

    def send_blocks(key, sources, slot, target):
        made = []
        for k in range(3):
            index = hops[key] * 3 + k
            copy = remote(
                sources[k],
                gathered[k].at[slot],
                hop_send.at[index],
                hop_recv.at[index],
                target,
                mine,
            )
            copy.start()
            made.append(copy)
        hop_copies[key] = made

    def hop_on(name, hop):
        step = 1 if name[1] == "r" else circle - 1
        target = ((spot + step) % circle) * 2 + parity
        origin = ((spot + (hop - 1) * (circle - step)) % circle) * 2
        if name[0] == "o":
            slot = origin + parity
            sources = originals(parity) if hop == 1 else [ref.at[slot] for ref in gathered]
        else:
            slot = origin + 1 - parity
            sources = [ref.at[slot] for ref in gathered]
        send_blocks((name, hop), sources, slot, target)

    def landed(key):
        for copy in hop_copies[key]:
            copy.wait_recv()

    send_blocks("x", originals(1 - parity), me, partner)
    hop_on("or", 1)
    if near:
        hop_on("ol", 1)
    tokens = x_ref.shape[0]
    lanes = growth.shape[1]
    steps = tokens // SUB
    rows = lax.broadcasted_iota(jnp.int32, (tokens, tokens), 0)
    cols = lax.broadcasted_iota(jnp.int32, (tokens, tokens), 1)
    spread = (cols == (rows % SUB) * steps + rows // SUB).astype(bf16)
    gather = (rows == (cols % SUB) * steps + cols // SUB).astype(bf16)
    x_perm = jnp.dot(spread, x_ref[...], preferred_element_type=f32).astype(bf16)
    factor = jnp.exp(damp_ref[...])
    high = factor.astype(bf16)
    rest = factor - high.astype(f32)
    middle = rest.astype(bf16)
    low = (rest - middle.astype(f32)).astype(bf16)
    groups = factor.shape[1]
    pick = (
        lax.broadcasted_iota(jnp.int32, (groups, lanes), 1) // states
        == lax.broadcasted_iota(jnp.int32, (groups, lanes), 0)
    ).astype(bf16)
    total = None
    for part in (high, middle, low):
        moved = jnp.dot(spread, part, preferred_element_type=f32).astype(bf16)
        spanned = jnp.dot(moved, pick, preferred_element_type=f32)
        total = spanned if total is None else total + spanned
    growth[...] = total
    height = in_ref.shape[1]
    width = 128
    per_block = width // height
    span = per_block * states
    blocks = groups // per_block
    for b in range(blocks):
        piece = x_perm[:, b * width : (b + 1) * width]
        cut = slice(b * span, (b + 1) * span)
        f_re, f_im = (factor_re_ref[:, cut], factor_im_ref[:, cut])
        m_re, m_im = (in_ref[0, :, cut], in_ref[1, :, cut])
        bbar_re = diagonal(f_re * m_re - f_im * m_im, per_block, height, states)
        bbar_im = diagonal(f_re * m_im + f_im * m_re, per_block, height, states)
        state_re[:, cut] = jnp.dot(piece, bbar_re, preferred_element_type=f32)
        state_im[:, cut] = jnp.dot(piece, bbar_im, preferred_element_type=f32)

    def advance(start, keep, cut, re, im, a_re, a_im):
        row = pl.multiple_of(start * SUB, SUB)
        grow = growth[pl.ds(row, SUB), cut]
        re, im = (re * grow, im * grow)
        new_re = a_re * re - a_im * im + state_re[pl.ds(row, SUB), cut]
        new_im = a_re * im + a_im * re + state_im[pl.ds(row, SUB), cut]
        if keep:
            state_re[pl.ds(row, SUB), cut] = new_re
            state_im[pl.ds(row, SUB), cut] = new_im
        return (new_re, new_im, grow)

    total_re, total_im = complex_power(abar_re_ref[...], abar_im_ref[...], steps)
    local = []
    for lane in range(0, lanes, LANE_BLOCK):
        cut = slice(lane, lane + LANE_BLOCK)
        a_re = jnp.broadcast_to(abar_re_ref[:, cut], (SUB, LANE_BLOCK))
        a_im = jnp.broadcast_to(abar_im_ref[:, cut], (SUB, LANE_BLOCK))

        def body(step, carry):
            re, im, grown = carry
            re, im, grow = advance(step, False, cut, re, im, a_re, a_im)
            return (re, im, grown * grow)

        zero = jnp.zeros((SUB, LANE_BLOCK), f32)
        re, im, grown = lax.fori_loop(
            0, steps, body, (zero, zero, jnp.ones((SUB, LANE_BLOCK), f32)), unroll=4
        )
        local.append((re, im, grown * total_re[:, cut], grown * total_im[:, cut]))
    fin_re, fin_im, jump_re, jump_im = [
        jnp.concatenate([item[k] for item in local], axis=1) for k in range(4)
    ]
    at_re, at_im = (fin_re[0:1], fin_im[0:1])
    all_re, all_im = (jump_re[0:1], jump_im[0:1])
    for c in range(1, SUB):
        j_re, j_im = (jump_re[c : c + 1], jump_im[c : c + 1])
        at_re, at_im = (
            j_re * at_re - j_im * at_im + fin_re[c : c + 1],
            j_re * at_im + j_im * at_re + fin_im[c : c + 1],
        )
        all_re, all_im = (j_re * all_re - j_im * all_im, j_re * all_im + j_im * all_re)
    outbox[0:1, :] = at_re
    outbox[1:2, :] = at_im
    outbox[2:3, :] = all_re
    outbox[3:4, :] = all_im
    copies = []
    for apart in range(1, ring):
        copy = remote(
            outbox,
            inbox.at[apart],
            send_sem.at[apart],
            recv_sem.at[apart],
            lax.rem(me + apart, ring),
            mine,
        )
        copy.start()
        copies.append(copy)
    for copy in copies:
        copy.wait()
    at_re = jnp.zeros((1, lanes), f32)
    at_im = jnp.zeros((1, lanes), f32)
    for apart in range(ring - 1, 0, -1):
        f_re, f_im = (inbox[apart, 0:1, :], inbox[apart, 1:2, :])
        j_re, j_im = (inbox[apart, 2:3, :], inbox[apart, 3:4, :])
        valid = me >= apart
        new_re = j_re * at_re - j_im * at_im + f_re
        new_im = j_re * at_im + j_im * at_re + f_im
        at_re = jnp.where(valid, new_re, at_re)
        at_im = jnp.where(valid, new_im, at_im)
    for c in range(SUB):
        begin_re[c : c + 1, :] = at_re
        begin_im[c : c + 1, :] = at_im
        if c < SUB - 1:
            j_re, j_im = (jump_re[c : c + 1], jump_im[c : c + 1])
            at_re, at_im = (
                j_re * at_re - j_im * at_im + fin_re[c : c + 1],
                j_re * at_im + j_im * at_re + fin_im[c : c + 1],
            )
    for lane in range(0, lanes, LANE_BLOCK):
        cut = slice(lane, lane + LANE_BLOCK)
        a_re = jnp.broadcast_to(abar_re_ref[:, cut], (SUB, LANE_BLOCK))
        a_im = jnp.broadcast_to(abar_im_ref[:, cut], (SUB, LANE_BLOCK))

        def body(step, carry):
            re, im, _ = advance(step, True, cut, *carry, a_re, a_im)
            return (re, im)

        lax.fori_loop(0, steps, body, (begin_re[:, cut], begin_im[:, cut]), unroll=4)

    def across(state, compact):
        return lax.dot_general(
            state,
            diagonal(compact, per_block, height, states),
            (((1,), (1,)), ((), ())),
            preferred_element_type=f32,
        )

    landed("x")
    if near:
        hop_on("pr", 1)
    hop_on("pl", 1)
    if far > 1:
        landed(("or", 1))
        hop_on("or", 2)
    pieces = []
    for b in range(blocks):
        cut = slice(b * span, (b + 1) * span)
        here = slice(b * width, (b + 1) * width)
        mixed = (
            across(state_re[:, cut].astype(bf16), out_ref[0, :, cut])
            - across(state_im[:, cut].astype(bf16), out_ref[1, :, cut])
            + skip_ref[:, here] * x_perm[:, here].astype(f32)
        )
        pieces.append(jax.nn.gelu(mixed).astype(bf16))
    activated = jnp.dot(
        gather, jnp.concatenate(pieces, axis=1), preferred_element_type=f32
    ).astype(bf16)
    columns = w_out_ref.shape[1]
    piece = min(512, columns)

    def project(k, _):
        there = pl.ds(pl.multiple_of(k * piece, piece), piece)
        proj[:, there] = jnp.dot(
            activated, w_out_ref[:, there], preferred_element_type=f32
        ).astype(bf16)
        return 0

    lax.fori_loop(0, columns // piece, project, 0)
    share = tokens // team
    sums = []
    for apart in range(1, team):
        other = lax.rem(mine + apart, team)
        copy = remote(
            proj.at[pl.ds(pl.multiple_of(other * share, share), share), :],
            rs_in.at[apart],
            rs_send.at[apart],
            rs_recv.at[apart],
            me,
            other,
        )
        copy.start()
        sums.append(copy)
    stores = []
    for k in range(3):
        loads[k].wait()
        store = pltpu.make_async_copy(keep[k], gathered[k].at[me], local_sem.at[3 + k])
        store.start()
        stores.append(store)
    for copy in sums:
        copy.wait()
    total = proj[pl.ds(pl.multiple_of(mine * share, share), share), :].astype(f32)
    for apart in range(1, team):
        total = total + rs_in[apart].astype(f32)
    stream = (residual_ref[...].astype(f32) + total).astype(bf16)
    stream_ref[...] = stream
    stream = stream.astype(f32)
    scale = lax.rsqrt(jnp.mean(stream * stream, axis=-1, keepdims=True) + 1e-06)
    place = pl.ds(pl.multiple_of(parity * tokens + mine * share, share), share)
    pair_ref[place, :] = (stream * scale * gain_ref[...]).astype(bf16)
    sibling = mine + 1 - 2 * (mine % 2)
    spread_copies = []

    def send_rows(owner_sp, owner_tp, at_sp, at_tp):
        k = len(spread_copies)
        start = (owner_sp % 2) * tokens + owner_tp * share
        here = pair_ref.at[pl.ds(pl.multiple_of(start, share), share), :]
        copy = remote(here, here, ag_send.at[k], ag_recv.at[k], at_sp, at_tp)
        copy.start()
        spread_copies.append(copy)

    send_rows(me, mine, partner, mine)
    owners = [(partner, mine)]
    for apart in range(2, team, 2):
        to_tp, from_tp = (lax.rem(mine + apart, team), lax.rem(mine + team - apart, team))
        for side in (me, partner):
            send_rows(me, mine, side, to_tp)
            owners.append((side, from_tp))
    send_rows(me, mine, me, sibling)
    for k, owner in enumerate(owners):
        spread_copies[k].wait_recv()
        send_rows(*owner, me, sibling)
    if far > 1:
        landed(("pl", 1))
        hop_on("pl", 2)
    if near > 1:
        landed(("ol", 1))
        hop_on("ol", 2)
        landed(("pr", 1))
        hop_on("pr", 2)
    for hop in range(3, far + 1):
        for name in ("or", "pl", "ol", "pr"):
            if (name, hop) in hops:
                landed((name, hop - 1))
                hop_on(name, hop)
    forwarded = {("or", h) for h in range(1, far)} | {("pl", h) for h in range(1, far)}
    forwarded |= {("ol", h) for h in range(1, near)} | {("pr", h) for h in range(1, near)} | {"x"}
    for k, copy in enumerate(spread_copies):
        copy.wait_send()
        if k >= len(owners):
            copy.wait_recv()
    for key, made in hop_copies.items():
        for copy in made:
            copy.wait_send()
            if key not in forwarded:
                copy.wait_recv()
    for store in stores:
        store.wait()


def exit_kernel(
    ring, team, hidden_ref, down_ref, stream_ref, out_ref, outbox, inbox, send_sem, recv_sem
):
    f32 = jnp.float32
    me, mine = (lax.axis_index("sp"), lax.axis_index("tp"))
    partner = me + 1 - 2 * (me % 2)
    barrier = pltpu.get_barrier_semaphore()
    rows = out_ref.shape[0]
    peers = [(partner, lax.rem(mine + apart, team)) for apart in range(team)]
    peers += [(me, lax.rem(mine + apart, team)) for apart in range(1, team)]
    for at_sp, at_tp in peers:
        pl.semaphore_signal(
            barrier, inc=1, device_id={"sp": at_sp, "tp": at_tp}, device_id_type=MESH
        )
    columns = down_ref.shape[1]
    piece = min(512, columns)

    def product(slot, at_sp, at_tp):
        start = pl.multiple_of(((at_sp % 2) * team + at_tp) * rows, rows)
        block = hidden_ref[pl.ds(start, rows), :]

        def some(k, _):
            there = pl.ds(pl.multiple_of(k * piece, piece), piece)
            outbox[slot, :, there] = jnp.dot(
                block, down_ref[:, there], preferred_element_type=f32
            ).astype(jnp.bfloat16)
            return 0

        lax.fori_loop(0, columns // piece, some, 0)

    copies = []
    order = sorted(range(len(peers)), key=lambda k: (k >= team, -(k % team)))
    for k in order:
        product(k, *peers[k])
        if not copies:
            pl.semaphore_wait(barrier, len(peers))
        copy = remote(outbox.at[k], inbox.at[k], send_sem.at[k], recv_sem.at[k], *peers[k])
        copy.start()
        copies.append(copy)
    product(len(peers), me, mine)
    for copy in copies:
        copy.wait()
    total = outbox[len(peers)].astype(f32)
    for k in range(len(peers)):
        total = total + inbox[k].astype(f32)
    out_ref[...] = (stream_ref[...].astype(f32) + total).astype(jnp.bfloat16)


def enter_layer(
    mixer_input,
    residual,
    log_step,
    rate_real,
    rate_imag,
    damping,
    in_map,
    out_map,
    skip,
    w_out,
    norm_gain,
    w_act,
    w_lin,
    w_down,
    wide,
):
    tokens_here, channels = mixer_input.shape
    groups_here, states = rate_real.shape
    step_size = jnp.exp(log_step)[:, None]
    log_rate = rate_real * step_size
    angle_step = rate_imag * step_size
    magnitude = jnp.exp(log_rate)
    abar_re = magnitude * jnp.cos(angle_step)
    abar_im = magnitude * jnp.sin(angle_step)
    denominator = rate_real * rate_real + rate_imag * rate_imag
    minus_one = abar_re - 1.0
    factor_re = (minus_one * rate_real + abar_im * rate_imag) / denominator
    factor_im = (abar_im * rate_real - minus_one * rate_imag) / denominator
    lanes = groups_here * states
    ring, team = (lax.axis_size("sp"), lax.axis_size("tp"))
    width = w_out.shape[1]
    vmem = pl.BlockSpec(memory_space=pltpu.VMEM)
    anywhere = pl.BlockSpec(memory_space=pl.ANY)
    f32, bf16 = (jnp.float32, jnp.bfloat16)
    group_width = channels // groups_here
    dma = pltpu.SemaphoreType.DMA
    hop_count = 3 * (1 + 2 * (ring // 2 - 1))
    return pl.pallas_call(
        functools.partial(entry_kernel, ring, team, states),
        out_shape=(
            jax.ShapeDtypeStruct((tokens_here // team, width), bf16),
            jax.ShapeDtypeStruct((2 * tokens_here, width), bf16),
            jax.ShapeDtypeStruct((ring, w_act.shape[0], wide), bf16),
            jax.ShapeDtypeStruct((ring, w_lin.shape[0], wide), bf16),
            jax.ShapeDtypeStruct((ring, wide, w_down.shape[1]), bf16),
        ),
        in_specs=[vmem] * 12 + [anywhere] * 3,
        out_specs=(vmem, vmem, anywhere, anywhere, anywhere),
        scratch_shapes=[
            pltpu.VMEM((tokens_here, lanes), f32),
            pltpu.VMEM((tokens_here, lanes), f32),
            pltpu.VMEM((tokens_here, lanes), f32),
            pltpu.VMEM((SUB, lanes), f32),
            pltpu.VMEM((SUB, lanes), f32),
            pltpu.VMEM((4, lanes), f32),
            pltpu.VMEM((ring, 4, lanes), f32),
            pltpu.VMEM((tokens_here, width), bf16),
            pltpu.VMEM((team, tokens_here // team, width), bf16),
            pltpu.VMEM((2, w_act.shape[0], wide), bf16),
            pltpu.VMEM((wide, w_down.shape[1]), bf16),
            dma((ring,)),
            dma((ring,)),
            dma((team,)),
            dma((team,)),
            dma((2 * team - 1,)),
            dma((2 * team - 1,)),
            dma((hop_count,)),
            dma((hop_count,)),
            dma((6,)),
        ],
        compiler_params=pltpu.CompilerParams(
            collective_id=0, has_side_effects=True, vmem_limit_bytes=56 * 1024 * 1024
        ),
        cost_estimate=pl.CostEstimate(
            flops=20_000_000_000, bytes_accessed=8_000_000, transcendentals=0
        ),
        name="enter_layer",
    )(
        mixer_input,
        damping,
        abar_re.reshape(1, lanes),
        abar_im.reshape(1, lanes),
        factor_re.reshape(1, lanes),
        factor_im.reshape(1, lanes),
        jnp.transpose(in_map, (0, 3, 1, 2)).reshape(2, group_width, lanes),
        jnp.transpose(out_map, (0, 2, 1, 3)).reshape(2, group_width, lanes),
        skip.reshape(1, channels),
        w_out,
        residual,
        norm_gain.reshape(1, width),
        w_act,
        w_lin,
        w_down,
    )


def leave_layer(hidden, down, stream):
    ring, team = (lax.axis_size("sp"), lax.axis_size("tp"))
    rows, width = stream.shape
    vmem = pl.BlockSpec(memory_space=pltpu.VMEM)
    return pl.pallas_call(
        functools.partial(exit_kernel, ring, team),
        out_shape=jax.ShapeDtypeStruct((rows, width), jnp.bfloat16),
        in_specs=[vmem] * 3,
        out_specs=vmem,
        scratch_shapes=[
            pltpu.VMEM((2 * team, rows, width), jnp.bfloat16),
            pltpu.VMEM((2 * team - 1, rows, width), jnp.bfloat16),
            pltpu.SemaphoreType.DMA((2 * team - 1,)),
            pltpu.SemaphoreType.DMA((2 * team - 1,)),
        ],
        compiler_params=pltpu.CompilerParams(
            collective_id=1, has_side_effects=True, vmem_limit_bytes=48 * 1024 * 1024
        ),
        cost_estimate=pl.CostEstimate(
            flops=20_000_000_000, bytes_accessed=8_000_000, transcendentals=0
        ),
        name="leave_layer",
    )(hidden, down, stream)


def from_behind(value, axis, steps):
    count = lax.axis_size(axis)
    initial, last = (max(0, -steps), min(count, count - steps))
    return lax.ppermute(value, axis, [(source, source + steps) for source in range(initial, last)])


def causal_conv(act_pre, lin_pre, previous, taps):
    row_count, width = act_pre.shape
    act_pad = jnp.concatenate([previous[0], act_pre], axis=0).astype(jnp.float32)
    lin_pad = jnp.concatenate([previous[1], lin_pre], axis=0).astype(jnp.float32)
    act_conv = jnp.zeros((row_count, width), jnp.float32)
    lin_conv = jnp.zeros((row_count, width), jnp.float32)
    for offset in range(CONV):
        act_conv = act_conv + taps[0, offset][None, :] * act_pad[offset : offset + row_count]
        lin_conv = lin_conv + taps[1, offset][None, :] * lin_pad[offset : offset + row_count]
    return (jax.nn.silu(act_conv) * lin_conv).astype(jnp.bfloat16)


def per_device(
    mixer_input,
    residual,
    log_step,
    rate_real,
    rate_imag,
    damping,
    in_map,
    out_map,
    skip,
    w_out,
    norm_gain,
    w_act,
    w_lin,
    conv_taps,
    w_down,
):
    tokens_here = mixer_input.shape[0]
    hidden_here = w_act.shape[1]
    wide = -(-hidden_here // 256) * 128
    parity = lax.axis_index("sp") % 2
    stream, normed_pair, act_all, lin_all, down_all = enter_layer(
        mixer_input,
        residual,
        log_step,
        rate_real,
        rate_imag,
        damping,
        in_map,
        out_map,
        skip,
        w_out,
        norm_gain,
        w_act,
        w_lin,
        w_down,
        wide,
    )
    act_half = act_all.reshape(-1, wide)
    lin_half = lin_all.reshape(-1, wide)
    down_half = jnp.transpose(down_all, (1, 0, 2)).reshape(wide, -1)
    act_pre = jnp.dot(normed_pair, act_half, preferred_element_type=jnp.float32).astype(
        jnp.bfloat16
    )
    lin_pre = jnp.dot(normed_pair, lin_half, preferred_element_type=jnp.float32).astype(
        jnp.bfloat16
    )
    edge = 2 * tokens_here - (CONV - 1)
    previous = from_behind((act_pre[edge:], lin_pre[edge:]), "sp", 2)
    taps = lax.dynamic_slice_in_dim(conv_taps, parity * (hidden_here - wide), wide, 2)
    hidden = causal_conv(act_pre, lin_pre, previous, taps)
    doubled = parity * (2 * wide - hidden_here)
    hidden = jnp.where(jnp.arange(wide)[None, :] >= doubled, hidden, jnp.zeros_like(hidden))
    return leave_layer(hidden, down_half, stream)


def solution(mesh):
    in_specs = (
        P("sp", "tp"),
        P(("sp", "tp"), None),
        P("tp"),
        P("tp", None),
        P("tp", None),
        P("sp", "tp"),
        P(None, "tp", None, None),
        P(None, "tp", None, None),
        P("tp"),
        P("tp", None),
        P(),
        P("sp", "tp"),
        P("sp", "tp"),
        P(None, None, "tp"),
        P("tp", "sp"),
    )
    out_specs = P(("sp", "tp"), None)
    return jax.shard_map(
        per_device, mesh=mesh, in_specs=in_specs, out_specs=out_specs, check_vma=False
    )
```
